32 devices in a mesh: grp: 2 (over y), dp: 2 (over x), kv: 4 (over z), tp: 2 (over core).
Axes of the slice: x: 2, y: 2, z: 4, core: 2. Of those that a mesh axis runs over, the one named last changes fastest.
Arguments:
- residual_input: bfloat16 [128, 4096], P(('grp', 'dp', 'tp'), 'kv'), parts along dimension 0, may hold values from -6 to 6
- incoming_state: float32 [128, 16, 64, 128], P(('grp', 'kv'), ('dp', 'tp')), parts along dimension 0, may hold values from -4 to 4
- extra_log_decay: float32 [128, 1024], P(('grp', 'kv'), ('dp', 'tp')), parts along dimension 0, may hold values from -0.7 to 0
- leading_norm_gain: float32 [4096], P('kv'), may hold values from 0.1 to 1.9
- leading_gate_weight: bfloat16 [4096, 11264], P('kv', ('dp', 'tp')), may hold values from -0.09375 to 0.09375
- leading_up_weight: bfloat16 [4096, 11264], P('kv', ('dp', 'tp')), may hold values from -0.09375 to 0.09375
- leading_down_weight: bfloat16 [11264, 4096], P(('dp', 'tp'), 'kv'), may hold values from -0.0546875 to 0.0546875
- attention_norm_gain: float32 [4096], P('kv'), may hold values from 0.1 to 1.9
- query_projector: bfloat16 [4096, 1024], P('kv', ('dp', 'tp')), may hold values from -0.09375 to 0.09375
- key_projector: bfloat16 [4096, 1024], P('kv', ('dp', 'tp')), may hold values from -0.09375 to 0.09375
- value_projector: bfloat16 [4096, 2048], P('kv', ('dp', 'tp')), may hold values from -0.09375 to 0.09375
- output_gate_weight: bfloat16 [4096, 2048], P('kv', ('dp', 'tp')), may hold values from -0.09375 to 0.09375
- forget_weight: bfloat16 [4096, 1024], P('kv', ('dp', 'tp')), may hold values from -0.75 to 0.75
- head_norm_gain: float32 [128], replicated, may hold values from 0.1 to 1.9
- output_projector: bfloat16 [2048, 4096], P(('dp', 'tp'), 'kv'), may hold values from -0.125 to 0.125
- trailing_norm_gain: float32 [4096], P('kv'), may hold values from 0.1 to 1.9
- trailing_gate_weight: bfloat16 [4096, 11264], P('kv', ('dp', 'tp')), may hold values from -0.09375 to 0.09375
- trailing_up_weight: bfloat16 [4096, 11264], P('kv', ('dp', 'tp')), may hold values from -0.09375 to 0.09375
- trailing_down_weight: bfloat16 [11264, 4096], P(('dp', 'tp'), 'kv'), may hold values from -0.0546875 to 0.0546875
Outputs:
- result: bfloat16 [128, 4096], P(('grp', 'dp', 'tp'), 'kv'), parts along dimension 0
- new_state: float32 [128, 16, 64, 128], P(('grp', 'kv'), ('dp', 'tp')), parts along dimension 0
The draws below stay inside these ranges and needn't reach their ends.
There are 2 independent parts, one for each index of `grp`. The reference program is written for one: setup_inputs(seed, part) draws one part's arguments, and reference() takes and returns one part's arrays. A program takes and returns all parts, laid end to end along the dimension named above; an argument that names none is the same for every part. Nothing has to cross between parts.
All inputs are finite; a program needn't handle non-finite values.
Results may differ from the reference program's by a relative error of at most 0.0095.
Values may be sent and summed in bfloat16 or wider, within the bound.
No kernel may reach another device: no remote copies, remote signals or barrier semaphores. Data moves between devices by JAX's collectives and lax.ppermute only.
A program may use at most 128 MiB of HBM per device.

```python
import jax
import jax.numpy as jnp
from jax import lax

D = 4096
FF = 11264
HEAD_COUNT = 16
KEY_CHANNELS = 64
VALUE_DIM = 128
BATCH_SIZE = 64


def shard_levels(stream_key, shape, split, low, largest):
    level, own = 1.0, jax.random.fold_in(stream_key, 6)
    for axis_at, parts in split:
        steps = jnp.exp(jax.random.uniform(jax.random.fold_in(own, axis_at), (parts,), jnp.float32, low / len(split), largest / len(split)))
        level = level * jnp.repeat(steps, shape[axis_at] // parts).reshape([-1 if axis == axis_at else 1 for axis in range(len(shape))])
    return level


def bell_draw(key, extent, spread, limit, cuts=(), held_as=jnp.bfloat16):
    factor_of = shard_levels(key, extent, cuts, -0.22, 0.18) if cuts else 1.0
    values = jax.random.normal(key, extent, jnp.float32) * spread * factor_of
    return jnp.minimum(jnp.maximum(values, -limit), limit).astype(held_as)


def setup_inputs(seed: int = 0, part: int = 0) -> dict:
    splits = jax.random.split(jax.random.key(seed), 20)
    own_keys = jax.random.split(jax.random.fold_in(splits[19], part), 20)
    return {
        "residual_input": bell_draw(own_keys[0], (BATCH_SIZE, D), 1.0, 6.0, ((0, 4), (1, 4))),
        "incoming_state": bell_draw(own_keys[1], (BATCH_SIZE, HEAD_COUNT, KEY_CHANNELS, VALUE_DIM), 0.5, 4.0, ((0, 4), (1, 4)), jnp.float32),
        "extra_log_decay": jnp.clip(-0.7 + 0.7 * jax.random.uniform(own_keys[2], (BATCH_SIZE, HEAD_COUNT * KEY_CHANNELS), jnp.float32) ** shard_levels(own_keys[2], (BATCH_SIZE, HEAD_COUNT * KEY_CHANNELS), ((0, 4), (1, 4)), -0.2, 0.2), -0.7, 0.0),
        "leading_norm_gain": jnp.clip(1.0 + 0.18 * jax.random.normal(splits[3], (D,), jnp.float32), 0.1, 1.9),
        "leading_gate_weight": bell_draw(splits[4], (D, FF), D ** -0.5, 0.09375, ((0, 4), (1, 4))),
        "leading_up_weight": bell_draw(splits[5], (D, FF), D ** -0.5, 0.09375, ((0, 4), (1, 4))),
        "leading_down_weight": bell_draw(splits[6], (FF, D), FF ** -0.5, 0.0546875, ((0, 4), (1, 4))),
        "attention_norm_gain": jnp.clip(1.0 + 0.18 * jax.random.normal(splits[7], (D,), jnp.float32), 0.1, 1.9),
        "query_projector": bell_draw(splits[8], (D, HEAD_COUNT * KEY_CHANNELS), D ** -0.5, 0.09375, ((0, 4), (1, 4))),
        "key_projector": bell_draw(splits[9], (D, HEAD_COUNT * KEY_CHANNELS), D ** -0.5, 0.09375, ((0, 4), (1, 4))),
        "value_projector": bell_draw(splits[10], (D, HEAD_COUNT * VALUE_DIM), D ** -0.5, 0.09375, ((0, 4), (1, 4))),
        "output_gate_weight": bell_draw(splits[11], (D, HEAD_COUNT * VALUE_DIM), D ** -0.5, 0.09375, ((0, 4), (1, 4))),
        "forget_weight": bell_draw(splits[12], (D, HEAD_COUNT * KEY_CHANNELS), (max(D // 64, 1)) ** -0.5, 0.75, ((0, 4), (1, 4))),
        "head_norm_gain": jnp.clip(1.0 + 0.18 * jax.random.normal(splits[13], (VALUE_DIM,), jnp.float32), 0.1, 1.9),
        "output_projector": bell_draw(splits[14], (HEAD_COUNT * VALUE_DIM, D), (HEAD_COUNT * VALUE_DIM) ** -0.5, 0.125, ((0, 4), (1, 4))),
        "trailing_norm_gain": jnp.clip(1.0 + 0.18 * jax.random.normal(splits[15], (D,), jnp.float32), 0.1, 1.9),
        "trailing_gate_weight": bell_draw(splits[16], (D, FF), D ** -0.5, 0.09375, ((0, 4), (1, 4))),
        "trailing_up_weight": bell_draw(splits[17], (D, FF), D ** -0.5, 0.09375, ((0, 4), (1, 4))),
        "trailing_down_weight": bell_draw(splits[18], (FF, D), FF ** -0.5, 0.0546875, ((0, 4), (1, 4))),
    }


epsilon = 1e-06

def row_scale(row_block):
    widened = row_block.astype(jnp.float32)
    return lax.rsqrt(lax.optimization_barrier(jnp.sum(widened * widened, axis=1, keepdims=True)) / D + epsilon)

def channel_mixer(row_block, norm_gain, gate_matrix, up_matrix, down_matrix):
    decay_factor = row_scale(row_block)
    scaled = (row_block.astype(jnp.float32) * norm_gain).astype(jnp.bfloat16)
    gate_sum = decay_factor * jnp.dot(scaled, gate_matrix, preferred_element_type=jnp.float32)
    up_sum = decay_factor * jnp.dot(scaled, up_matrix, preferred_element_type=jnp.float32)
    hidden = (jax.nn.silu(gate_sum) * up_sum).astype(jnp.bfloat16)
    return jnp.dot(hidden, down_matrix, preferred_element_type=jnp.float32)

def reference(residual_input, incoming_state, extra_log_decay, leading_norm_gain, leading_gate_weight, leading_up_weight, leading_down_weight, attention_norm_gain, query_projector, key_projector, value_projector, output_gate_weight, forget_weight, head_norm_gain, output_projector, trailing_norm_gain, trailing_gate_weight, trailing_up_weight, trailing_down_weight):
    after_first = (residual_input.astype(jnp.float32) + 0.5 * channel_mixer(residual_input, leading_norm_gain, leading_gate_weight, leading_up_weight, leading_down_weight)).astype(jnp.bfloat16)
    decay_factor = row_scale(after_first)
    scaled = (after_first.astype(jnp.float32) * attention_norm_gain).astype(jnp.bfloat16)

    def apply_projection(matrix):
        return decay_factor * jnp.dot(scaled, matrix, preferred_element_type=jnp.float32)
    queries = apply_projection(query_projector).reshape(BATCH_SIZE, HEAD_COUNT, KEY_CHANNELS) * KEY_CHANNELS ** (-0.5)
    key_rows = apply_projection(key_projector).reshape(BATCH_SIZE, HEAD_COUNT, KEY_CHANNELS)
    value_rows = apply_projection(value_projector).reshape(BATCH_SIZE, HEAD_COUNT, VALUE_DIM)
    gate_rows = apply_projection(output_gate_weight).reshape(BATCH_SIZE, HEAD_COUNT, VALUE_DIM)
    decay_logarithm = (jax.nn.log_sigmoid(apply_projection(forget_weight)) / 16.0 + extra_log_decay).reshape(BATCH_SIZE, HEAD_COUNT, KEY_CHANNELS)
    new_state = jnp.exp(decay_logarithm)[..., None] * incoming_state + key_rows[..., None] * value_rows[:, :, None, :]
    read_out = jnp.einsum('bhk,bhkv->bhv', queries, new_state, precision=lax.Precision.HIGHEST)
    normed = read_out * lax.rsqrt(lax.optimization_barrier(jnp.mean(read_out * read_out, axis=-1, keepdims=True)) + epsilon)
    head_rows = (normed * head_norm_gain * jax.nn.silu(gate_rows)).astype(jnp.bfloat16).reshape(BATCH_SIZE, HEAD_COUNT * VALUE_DIM)
    second = (after_first.astype(jnp.float32) + jnp.dot(head_rows, output_projector, preferred_element_type=jnp.float32)).astype(jnp.bfloat16)
    result = (second.astype(jnp.float32) + 0.5 * channel_mixer(second, trailing_norm_gain, trailing_gate_weight, trailing_up_weight, trailing_down_weight)).astype(jnp.bfloat16)
    return (result, new_state)
```

```python
import functools

import jax
import jax.numpy as jnp
from jax import lax
from jax.experimental import pallas as pl
from jax.experimental.pallas import tpu as pltpu
from jax.sharding import PartitionSpec as P

KEY_CHANNELS = 64
VALUE_DIM = 128
EPSILON = 1e-06
LANES = 128
F32 = jnp.float32
BF16 = jnp.bfloat16

VMEM = pl.BlockSpec(memory_space=pltpu.VMEM)
HBM = pl.BlockSpec(memory_space=pl.ANY)


def padded(width):
    return -(-width // LANES) * LANES


def column_step(width):
    return 256 if width % 256 == 0 else width


def linear_index(axes):
    place = 0
    for axis in axes:
        place = place * lax.axis_size(axis) + lax.axis_index(axis)
    return place


def rows_at(block, height):
    return pl.ds(pl.multiple_of(block * height, height), height)


def swap(array, axes, size, offset):
    return lax.ppermute(array, axes, [(i, i ^ offset) for i in range(size)])


def swaps(arrays, axes, size):
    return [swap(array, axes, size, k + 1) for k, array in enumerate(arrays)]


def split_square_sum(rows):
    total = jnp.sum(rows * rows, axis=1, keepdims=True)
    high = total.astype(BF16)
    low = (total - high.astype(F32)).astype(BF16)
    lane = lax.broadcasted_iota(jnp.int32, (rows.shape[0], LANES), 1)
    return jnp.where(lane < LANES // 2, high.astype(F32), low.astype(F32)).astype(BF16)


def stream_columns(weights, buffers, semaphores):
    copies, at = [], 0
    for weight, buffer in zip(weights, buffers):
        width = weight.shape[1]
        step = column_step(width)
        pieces = []
        for low in range(0, width, step):
            piece = (slice(None), pl.ds(low, step))
            copy = pltpu.make_async_copy(weight.at[piece], buffer.at[piece], semaphores.at[at])
            copy.start()
            pieces.append((low, step, copy))
            at += 1
        copies.append(pieces)
    return copies


def count_pieces(weights):
    return sum(w.shape[1] // column_step(w.shape[1]) for w in weights)


def first_mixer_kernel(counts, *refs):
    n_dt, names = counts
    own, refs = refs[0], refs[1:]
    others, refs = refs[: n_dt - 1], refs[n_dt - 1 :]
    gain, gate, up = refs[:3]
    outs = refs[3 : 3 + n_dt]
    gathered = refs[3 + n_dt]
    gate_buffer, up_buffer, semaphores = refs[4 + n_dt :]
    copies = stream_columns((gate, up), (gate_buffer, up_buffer), semaphores)
    height = own.shape[0]
    dt_axes, kv_axes = names
    place = linear_index(dt_axes) ^ linear_index(kv_axes)
    for k, block in enumerate((own, *others)):
        gathered[rows_at(place ^ k, height), :] = block[...]
    widened = gathered[...].astype(F32)
    mix_rows(widened, gain, (gate_buffer, up_buffer), copies, outs)


def mix_rows(widened, gain, buffers, copies, outs):
    scaled = (widened * gain[...]).astype(BF16)
    height = outs[0].shape[0]
    base = 0
    for buffer, pieces in zip(buffers, copies):
        for low, step, copy in pieces:
            copy.wait()
            product = jnp.dot(scaled, buffer[:, low : low + step], preferred_element_type=F32).astype(BF16)
            for k, out in enumerate(outs):
                out[:, base + low : base + low + step] = product[k * height : (k + 1) * height]
        base += padded(buffer.shape[1])
    squares = split_square_sum(widened)
    for k, out in enumerate(outs):
        out[:, base : base + LANES] = squares[k * height : (k + 1) * height]


def project_kernel(half, n_parts, n_weights, n_outs, *refs):
    residual, refs = refs[0], refs[1:]
    parts, refs = refs[:n_parts], refs[n_parts:]
    gain, refs = refs[0], refs[1:]
    weights, refs = refs[:n_weights], refs[n_weights:]
    outs, refs = refs[:n_outs], refs[n_outs:]
    stream, refs = refs[0], refs[1:]
    buffers, semaphores = refs[:n_weights], refs[n_weights]
    copies = stream_columns(weights, buffers, semaphores)
    total = parts[0][...].astype(F32)
    for part in parts[1:]:
        total = total + part[...].astype(F32)
    rounded = (residual[...].astype(F32) + half * total).astype(BF16)
    stream[...] = rounded
    mix_rows(rounded.astype(F32), gain, buffers, copies, outs)


def hidden_kernel(features, n_parts, *refs):
    parts, out = refs[:n_parts], refs[n_parts]
    width = out.shape[1]
    gap = padded(width)

    def summed(low, size):
        total = parts[0][:, low : low + size].astype(F32)
        for part in parts[1:]:
            total = total + part[:, low : low + size].astype(F32)
        return total

    tail = summed(2 * gap, LANES)
    square_sum = tail[:, :1] + tail[:, LANES // 2 : LANES // 2 + 1]
    scale = lax.rsqrt(square_sum / features + EPSILON)
    step = column_step(width)
    for low in range(0, width, step):
        gate = scale * summed(low, step)
        up = scale * summed(gap + low, step)
        out[:, low : low + step] = (jax.nn.silu(gate) * up).astype(BF16)


def down_kernel(n_blocks, *refs):
    blocks, weight = refs[:n_blocks], refs[n_blocks]
    out, rows, buffer, semaphores = refs[n_blocks + 1 :]
    (pieces,) = stream_columns((weight,), (buffer,), semaphores)
    height = blocks[0].shape[0]
    for k, block in enumerate(blocks):
        rows[k * height : (k + 1) * height, :] = block[...]
    for low, step, copy in pieces:
        copy.wait()
        product = jnp.dot(rows[...], buffer[:, low : low + step], preferred_element_type=F32)
        out[:, low : low + step] = product.astype(BF16)


def attention_kernel(features, n_parts, *refs):
    parts, refs = refs[:n_parts], refs[n_parts:]
    extra_decay, state, norm_gain, head_rows, new_state, read, columns = refs
    rows, heads = state.shape[0], state.shape[1]
    keys, values = heads * KEY_CHANNELS, heads * VALUE_DIM
    gap, value_gap = padded(keys), padded(values)

    def summed(low, size):
        total = parts[0][:, low : low + size].astype(F32)
        for part in parts[1:]:
            total = total + part[:, low : low + size].astype(F32)
        return total

    tail = summed(3 * gap + 2 * value_gap, LANES)
    square_sum = tail[:, :1] + tail[:, LANES // 2 : LANES // 2 + 1]
    scale = lax.rsqrt(square_sum / features + EPSILON)
    queries = scale * summed(0, keys) * KEY_CHANNELS ** (-0.5)
    key_rows = scale * summed(gap, keys)
    forget = scale * summed(2 * gap, keys)
    value_rows = scale * summed(3 * gap, values)
    log_sigmoid = jnp.minimum(forget, 0.0) - jnp.log1p(jnp.exp(-jnp.abs(forget)))
    decay = jnp.exp(log_sigmoid / 16.0 + extra_decay[...])
    columns[...] = jnp.zeros_like(columns)
    columns[0:rows, :keys] = decay
    columns[rows : 2 * rows, :keys] = key_rows
    columns[2 * rows : 3 * rows, :keys] = queries
    upright = columns[...].T
    for head in range(heads):
        channels = slice(head * KEY_CHANNELS, (head + 1) * KEY_CHANNELS)
        lanes = slice(head * VALUE_DIM, (head + 1) * VALUE_DIM)
        for row in range(rows):
            kept = upright[channels, row : row + 1] * state[row, head]
            added = upright[channels, rows + row : rows + row + 1] * value_rows[row : row + 1, lanes]
            fresh = kept + added
            new_state[row, head] = fresh
            taken = upright[channels, 2 * rows + row : 2 * rows + row + 1] * fresh
            read[row : row + 1, lanes] = jnp.sum(taken, axis=0, keepdims=True)
    gates = scale * summed(3 * gap + value_gap, values)
    for head in range(heads):
        lanes = slice(head * VALUE_DIM, (head + 1) * VALUE_DIM)
        one = read[:, lanes]
        mean = jnp.mean(one * one, axis=-1, keepdims=True)
        normed = one * lax.rsqrt(mean + EPSILON) * norm_gain[...]
        head_rows[:, lanes] = (normed * jax.nn.silu(gates[:, lanes])).astype(BF16)


def result_kernel(n_parts, names, *refs):
    stream, parts, out = refs[0], refs[1 : 1 + n_parts], refs[1 + n_parts]
    total = parts[0][...].astype(F32)
    for part in parts[1:]:
        total = total + part[...].astype(F32)
    place = linear_index(names[0]) ^ linear_index(names[1])
    own = stream[rows_at(place, out.shape[0]), :].astype(F32)
    out[...] = (own + 0.5 * total).astype(BF16)


def scatter_down_kernel(n_blocks, names, *refs):
    blocks, weight = refs[:n_blocks], refs[n_blocks]
    outs = refs[n_blocks + 1 : 2 * n_blocks + 1]
    rows, product, buffer, semaphores = refs[2 * n_blocks + 1 :]
    (pieces,) = stream_columns((weight,), (buffer,), semaphores)
    height = blocks[0].shape[0]
    for k, block in enumerate(blocks):
        rows[k * height : (k + 1) * height, :] = block[...]
    place = linear_index(names[0]) ^ linear_index(names[1])
    for low, step, copy in pieces:
        copy.wait()
        product[...] = jnp.dot(rows[...], buffer[:, low : low + step], preferred_element_type=F32).astype(BF16)
        for k, out in enumerate(outs):
            out[:, low : low + step] = product[rows_at(place ^ k, height), :]


def call(kernel, name, outs, in_specs, scratch, limit):
    return pl.pallas_call(
        kernel,
        out_shape=outs,
        in_specs=in_specs,
        out_specs=jax.tree.map(lambda _: VMEM, outs),
        scratch_shapes=scratch,
        compiler_params=pltpu.CompilerParams(vmem_limit_bytes=limit),
        name=name,
    )


def weight_scratch(weights):
    return [pltpu.VMEM(w.shape, w.dtype) for w in weights] + [pltpu.SemaphoreType.DMA((count_pieces(weights),))]


def weight_bytes(weights):
    return sum(2 * w.shape[0] * padded(w.shape[1]) for w in weights)


MIB = 1 << 20


def per_device(
    n_dt,
    n_kv,
    residual_input,
    incoming_state,
    extra_log_decay,
    leading_norm_gain,
    leading_gate_weight,
    leading_up_weight,
    leading_down_weight,
    attention_norm_gain,
    query_projector,
    key_projector,
    value_projector,
    output_gate_weight,
    forget_weight,
    head_norm_gain,
    output_projector,
    trailing_norm_gain,
    trailing_gate_weight,
    trailing_up_weight,
    trailing_down_weight,
):
    dt, kv = ("dp", "tp"), ("kv",)
    names = (dt, kv)
    height, width = residual_input.shape
    features = width * n_kv
    rows = height * n_dt
    shape = jax.ShapeDtypeStruct

    def payload(weights):
        span = sum(padded(w.shape[1]) for w in weights) + LANES
        return [shape((height, span), BF16)] * n_kv

    def spread(block):
        return [block] + [swap(block, kv, n_kv, k) for k in range(1, n_kv)]

    def collect(blocks):
        return [blocks[0]] + swaps(blocks[1:], kv, n_kv)

    def total_parts(part):
        offset = 1
        while 2 * offset < n_dt:
            part = (part.astype(F32) + swap(part, dt, n_dt, offset).astype(F32)).astype(BF16)
            offset *= 2
        return [part, swap(part, dt, n_dt, offset)]

    def project_rows(half, residual, parts, gain, weights, name):
        return call(
            functools.partial(project_kernel, half, len(parts), len(weights), n_kv),
            name,
            payload(weights) + [shape((rows, width), BF16)],
            [VMEM] * (2 + len(parts)) + [HBM] * len(weights),
            weight_scratch(weights),
            weight_bytes(weights) + 12 * MIB,
        )(residual, *parts, gain.reshape(1, width), *weights)

    def hidden_rows(blocks, units):
        return call(
            functools.partial(hidden_kernel, features, n_kv),
            "hidden",
            shape((height, units), BF16),
            [VMEM] * n_kv,
            [],
            8 * MIB,
        )(*blocks)

    def down(blocks, weight, name):
        return call(
            functools.partial(down_kernel, n_kv),
            name,
            shape((rows, weight.shape[1]), BF16),
            [VMEM] * n_kv + [HBM],
            [pltpu.VMEM((rows, weight.shape[0]), BF16)] + weight_scratch((weight,)),
            weight_bytes((weight,)) + 8 * MIB,
        )(*blocks, weight)

    first = (leading_gate_weight, leading_up_weight)
    arrived = [swap(residual_input, dt, n_dt, k) for k in range(1, n_dt)]
    *blocks, gathered = call(
        functools.partial(first_mixer_kernel, (n_dt, names)),
        "first_mixer",
        payload(first) + [shape((rows, width), BF16)],
        [VMEM] * (n_dt + 1) + [HBM] * 2,
        weight_scratch(first),
        weight_bytes(first) + 12 * MIB,
    )(residual_input, *arrived, leading_norm_gain.reshape(1, width), *first)
    units = leading_gate_weight.shape[1]
    hidden = spread(hidden_rows(collect(blocks), units))
    parts = total_parts(down(hidden, leading_down_weight, "first_down"))

    mixed = (query_projector, key_projector, forget_weight, value_projector, output_gate_weight)
    *blocks, after_first = project_rows(0.5, gathered, parts, attention_norm_gain, mixed, "attention_in")
    blocks = collect(blocks)
    heads = incoming_state.shape[1]
    head_rows, new_state = call(
        functools.partial(attention_kernel, features, n_kv),
        "attention",
        [shape((height, heads * VALUE_DIM), BF16), shape(incoming_state.shape, F32)],
        [VMEM] * (n_kv + 3),
        [
            pltpu.VMEM((height, heads * VALUE_DIM), F32),
            pltpu.VMEM((padded(3 * height), padded(heads * KEY_CHANNELS)), F32),
        ],
        24 * MIB,
    )(*blocks, extra_log_decay, incoming_state, head_norm_gain.reshape(1, VALUE_DIM))
    parts = total_parts(down(spread(head_rows), output_projector, "attention_out"))

    last = (trailing_gate_weight, trailing_up_weight)
    *blocks, second = project_rows(1.0, after_first, parts, trailing_norm_gain, last, "last_mixer")
    hidden = spread(hidden_rows(collect(blocks), units))
    parts = call(
        functools.partial(scatter_down_kernel, n_kv, names),
        "last_down",
        [shape((height, width), BF16)] * n_dt,
        [VMEM] * n_kv + [HBM],
        [
            pltpu.VMEM((rows, trailing_down_weight.shape[0]), BF16),
            pltpu.VMEM((rows, column_step(width)), BF16),
        ]
        + weight_scratch((trailing_down_weight,)),
        weight_bytes((trailing_down_weight,)) + 8 * MIB,
    )(*hidden, trailing_down_weight)
    parts = [parts[0]] + swaps(parts[1:], dt, n_dt)
    result = call(
        functools.partial(result_kernel, n_dt, names),
        "result",
        shape((height, width), BF16),
        [VMEM] * (n_dt + 1),
        [],
        8 * MIB,
    )(second, *parts)
    return (result, new_state)


def solution(mesh):
    n_dt = mesh.shape["dp"] * mesh.shape["tp"]
    n_kv = mesh.shape["kv"]
    assert n_dt == n_kv and n_kv & (n_kv - 1) == 0
    return jax.shard_map(
        functools.partial(per_device, n_dt, n_kv),
        mesh=mesh,
        in_specs=(
            P(("grp", "dp", "tp"), "kv"),
            P(("grp", "kv"), ("dp", "tp"), None, None),
            P(("grp", "kv"), ("dp", "tp")),
            P("kv"),
            P("kv", ("dp", "tp")),
            P("kv", ("dp", "tp")),
            P(("dp", "tp"), "kv"),
            P("kv"),
            P("kv", ("dp", "tp")),
            P("kv", ("dp", "tp")),
            P("kv", ("dp", "tp")),
            P("kv", ("dp", "tp")),
            P("kv", ("dp", "tp")),
            P(),
            P(("dp", "tp"), "kv"),
            P("kv"),
            P("kv", ("dp", "tp")),
            P("kv", ("dp", "tp")),
            P(("dp", "tp"), "kv"),
        ),
        out_specs=(P(("grp", "dp", "tp"), "kv"), P(("grp", "kv"), ("dp", "tp"), None, None)),
        check_vma=False,
    )
```

```python
import functools

import jax
import jax.numpy as jnp
from jax import lax
from jax.experimental import pallas as pl
from jax.experimental.pallas import tpu as pltpu
from jax.sharding import PartitionSpec as P

KEY_CHANNELS = 64
VALUE_DIM = 128
EPSILON = 1e-06
LANES = 128
F32 = jnp.float32
BF16 = jnp.bfloat16

VMEM = pl.BlockSpec(memory_space=pltpu.VMEM)


def padded(width):
    return -(-width // LANES) * LANES


def column_step(width):
    return 256 if width % 256 == 0 else width


def linear_index(axes):
    place = 0
    for axis in axes:
        place = place * lax.axis_size(axis) + lax.axis_index(axis)
    return place


def rows_at(block, height):
    return pl.ds(pl.multiple_of(block * height, height), height)


def swap(array, axes, size, offset):
    return lax.ppermute(array, axes, [(i, i ^ offset) for i in range(size)])


def swaps(arrays, axes, size):
    return [swap(array, axes, size, k + 1) for k, array in enumerate(arrays)]


def split_square_sum(total):
    high = total.astype(BF16).astype(F32)
    lane = lax.broadcasted_iota(jnp.int32, (total.shape[0], LANES), 1)
    return jnp.where(lane < LANES // 2, high, total - high)


def join_square_sum(block):
    return block[:, :1] + block[:, LANES // 2 : LANES // 2 + 1]


def fetch_kernel(n_weights, *refs):
    weights, outs, semaphores = refs[:n_weights], refs[n_weights : 2 * n_weights], refs[-1]
    copies = []
    for weight, out in zip(weights, outs):
        step = weight.shape[0] // FETCH_PIECES
        for piece in range(FETCH_PIECES):
            part = pl.ds(piece * step, step)
            copies.append(pltpu.make_async_copy(weight.at[part], out.at[part], semaphores.at[len(copies)]))
            copies[-1].start()
    for copy in copies:
        copy.wait()


def multiply_blocks(scaled, weight, base, outs):
    height = outs[0].shape[0]
    width = weight.shape[1]
    step = column_step(width)
    for low in range(0, width, step):
        product = jnp.dot(scaled, weight[:, low : low + step], preferred_element_type=F32)
        for k, out in enumerate(outs):
            block = product[k * height : (k + 1) * height]
            out[:, base + low : base + low + step] = block.astype(out.dtype)


def put_squares(squares, low, outs):
    height = outs[0].shape[0]
    block = split_square_sum(squares)
    for k, out in enumerate(outs):
        out[:, low : low + LANES] = block[k * height : (k + 1) * height].astype(out.dtype)


def project_rows(widened, gain, weights, outs):
    scaled = (widened * gain[...]).astype(BF16)
    base = 0
    for weight in weights:
        multiply_blocks(scaled, weight, base, outs)
        base += padded(weight.shape[1])
    put_squares(jnp.sum(widened * widened, axis=1, keepdims=True), base, outs)


def first_kernel(n_dt, n_kv, names, *refs):
    own, others, refs = refs[0], refs[1:n_dt], refs[n_dt:]
    gain, weights, refs = refs[0], refs[1:3], refs[3:]
    outs, gathered = refs[:n_kv], refs[n_kv]
    height = own.shape[0]
    place = linear_index(names[0]) ^ linear_index(names[1])
    for k, block in enumerate((own, *others)):
        gathered[rows_at(place ^ k, height), :] = block[...]
    project_rows(gathered[...].astype(F32), gain, weights, outs)


def add_parts(residual, parts, half):
    total = parts[0][...].astype(F32)
    for part in parts[1:]:
        total = total + part[...].astype(F32)
    return (residual[...].astype(F32) + half * total).astype(BF16)


def project_kernel(half, n_parts, n_weights, *refs):
    residual, parts, refs = refs[0], refs[1 : 1 + n_parts], refs[1 + n_parts :]
    gain, weights, refs = refs[0], refs[1 : 1 + n_weights], refs[1 + n_weights :]
    outs, stream = refs[:-1], refs[-1]
    stream[...] = add_parts(residual, parts, half)
    project_rows(stream[...].astype(F32), gain, weights, outs)


def sum_columns(parts, low, size):
    total = parts[0][:, low : low + size].astype(F32)
    for part in parts[1:]:
        total = total + part[:, low : low + size].astype(F32)
    return total


def hidden_kernel(features, n_kv, *refs):
    parts, out = refs[:n_kv], refs[n_kv]
    width = out.shape[1]
    gap = padded(width)
    scale = lax.rsqrt(join_square_sum(sum_columns(parts, 2 * gap, LANES)) / features + EPSILON)
    step = column_step(width)
    for low in range(0, width, step):
        gate = jax.nn.silu(scale * sum_columns(parts, low, step))
        out[:, low : low + step] = (gate * (scale * sum_columns(parts, gap + low, step))).astype(BF16)


def stack_rows(blocks, rows):
    height = blocks[0].shape[0]
    for k, block in enumerate(blocks):
        rows[k * height : (k + 1) * height, :] = block[...]


def down_kernel(n_blocks, *refs):
    blocks, weight, (out, rows) = refs[:n_blocks], refs[n_blocks], refs[-2:]
    stack_rows(blocks, rows)
    step = column_step(weight.shape[1])
    for low in range(0, weight.shape[1], step):
        product = jnp.dot(rows[...], weight[:, low : low + step], preferred_element_type=F32)
        out[:, low : low + step] = product.astype(BF16)


def scatter_down_kernel(n_blocks, names, *refs):
    blocks, weight = refs[:n_blocks], refs[n_blocks]
    outs, (rows, product) = refs[n_blocks + 1 : -2], refs[-2:]
    stack_rows(blocks, rows)
    height = blocks[0].shape[0]
    place = linear_index(names[0]) ^ linear_index(names[1])
    step = column_step(weight.shape[1])
    for low in range(0, weight.shape[1], step):
        columns = slice(low, low + step)
        product[:, columns] = jnp.dot(rows[...], weight[:, columns], preferred_element_type=F32).astype(BF16)
    for k, out in enumerate(outs):
        out[...] = product[rows_at(place ^ k, height), :]


def attention_kernel(features, n_parts, *refs):
    parts, refs = refs[:n_parts], refs[n_parts:]
    extra_decay, state, norm_gain, head_rows, upright, value_rows, read, columns = refs
    rows, heads = state.shape[0], state.shape[1]
    keys, values = heads * KEY_CHANNELS, heads * VALUE_DIM
    gap, value_gap = padded(keys), padded(values)
    scale = lax.rsqrt(join_square_sum(sum_columns(parts, 3 * gap + 2 * value_gap, LANES)) / features + EPSILON)
    queries = scale * sum_columns(parts, 0, keys) * KEY_CHANNELS ** (-0.5)
    key_rows = scale * sum_columns(parts, gap, keys)
    forget = scale * sum_columns(parts, 2 * gap, keys)
    value_rows[...] = scale * sum_columns(parts, 3 * gap, values)
    log_sigmoid = jnp.minimum(forget, 0.0) - jnp.log1p(jnp.exp(-jnp.abs(forget)))
    decay = jnp.exp(log_sigmoid / 16.0 + extra_decay[...])
    columns[...] = jnp.zeros_like(columns)
    columns[0:rows, :keys] = decay
    columns[rows : 2 * rows, :keys] = key_rows
    columns[2 * rows : 3 * rows, :keys] = queries * decay
    upright[...] = columns[...].T
    matched = queries * key_rows
    for head in range(heads):
        channels = slice(head * KEY_CHANNELS, (head + 1) * KEY_CHANNELS)
        lanes = slice(head * VALUE_DIM, (head + 1) * VALUE_DIM)
        match = jnp.sum(matched[:, channels], axis=1, keepdims=True)
        for row in range(rows):
            taken = upright[channels, 2 * rows + row : 2 * rows + row + 1] * state[row, head]
            read[row : row + 1, lanes] = jnp.sum(taken, axis=0, keepdims=True)
        one = read[:, lanes] + match * value_rows[:, lanes]
        mean = jnp.mean(one * one, axis=-1, keepdims=True)
        normed = one * lax.rsqrt(mean + EPSILON) * norm_gain[...]
        low = 3 * gap + value_gap + head * VALUE_DIM
        gates = scale * sum_columns(parts, low, VALUE_DIM)
        head_rows[:, lanes] = (normed * jax.nn.silu(gates)).astype(BF16)


def state_kernel(upright, value_rows, state, new_state, finished):
    finished[...] = jnp.zeros_like(finished)
    rows, heads = state.shape[0], state.shape[1]
    for head in range(heads):
        channels = slice(head * KEY_CHANNELS, (head + 1) * KEY_CHANNELS)
        lanes = slice(head * VALUE_DIM, (head + 1) * VALUE_DIM)
        for row in range(rows):
            kept = upright[channels, row : row + 1] * state[row, head]
            added = upright[channels, rows + row : rows + row + 1] * value_rows[row : row + 1, lanes]
            new_state[row, head] = kept + added


def result_kernel(n_parts, names, *refs):
    stream, parts, out = refs[0], refs[1 : 1 + n_parts], refs[1 + n_parts]
    total = parts[0][...].astype(F32)
    for part in parts[1:]:
        total = total + part[...].astype(F32)
    place = linear_index(names[0]) ^ linear_index(names[1])
    own = stream[rows_at(place, out.shape[0]), :].astype(F32)
    out[...] = (own + 0.5 * total).astype(BF16)


MIB = 1 << 20
FETCH_PIECES = 4


def array_bytes(array):
    *lead, width = array.shape
    size = array.dtype.itemsize * padded(width)
    for extent in lead:
        size *= extent
    return size


def call(kernel, name, outs, inputs, scratch=(), in_specs=None, work=0, cores=8 * MIB):
    arrays = [*inputs, *jax.tree.leaves(outs)]
    return pl.pallas_call(
        kernel,
        out_shape=outs,
        in_specs=in_specs or [VMEM] * len(inputs),
        out_specs=jax.tree.map(lambda _: VMEM, outs),
        scratch_shapes=list(scratch),
        compiler_params=pltpu.CompilerParams(vmem_limit_bytes=sum(map(array_bytes, arrays)) + cores),
        cost_estimate=pl.CostEstimate(flops=work, bytes_accessed=0, transcendentals=0),
        name=name,
    )(*inputs)


def per_device(
    n_dt,
    n_kv,
    residual_input,
    incoming_state,
    extra_log_decay,
    leading_norm_gain,
    leading_gate_weight,
    leading_up_weight,
    leading_down_weight,
    attention_norm_gain,
    query_projector,
    key_projector,
    value_projector,
    output_gate_weight,
    forget_weight,
    head_norm_gain,
    output_projector,
    trailing_norm_gain,
    trailing_gate_weight,
    trailing_up_weight,
    trailing_down_weight,
):
    dt, kv = ("dp", "tp"), ("kv",)
    names = (dt, kv)
    height, width = residual_input.shape
    features = width * n_kv
    rows = height * n_dt
    shape = jax.ShapeDtypeStruct

    def collect(blocks):
        return [blocks[0]] + swaps(blocks[1:], kv, n_kv)

    def gather_rows(block):
        return [block] + [swap(block, kv, n_kv, k) for k in range(1, n_kv)]

    def total_parts(part):
        offset = 1
        while 2 * offset < n_dt:
            part = (part.astype(F32) + swap(part, dt, n_dt, offset).astype(F32)).astype(BF16)
            offset *= 2
        return [part, swap(part, dt, n_dt, offset)]

    def project(kernel, name, weights, inputs):
        span = sum(padded(w.shape[1]) for w in weights) + LANES
        outs = [shape((height, span), F32)] + [shape((height, span), BF16)] * (n_kv - 1)
        return call(kernel, name, outs + [shape((rows, width), BF16)], (*inputs, *weights))

    def hidden_rows(blocks, units):
        kernel = functools.partial(hidden_kernel, features, n_kv)
        return gather_rows(call(kernel, "hidden", shape((height, units), BF16), collect(blocks)))

    def down(blocks, weight, name, *after):
        kernel = functools.partial(down_kernel, n_kv)
        scratch = [pltpu.VMEM((rows, weight.shape[0]), BF16)]
        return call(kernel, name, shape((rows, weight.shape[1]), BF16), (*blocks, weight, *after), scratch)

    units = leading_gate_weight.shape[1]
    arrived = [swap(residual_input, dt, n_dt, k) for k in range(1, n_dt)]
    fetched = [
        pltpu.with_memory_space_constraint(w, pltpu.HBM) for w in (leading_gate_weight, leading_up_weight)
    ]
    gate, up = call(
        functools.partial(fetch_kernel, 2),
        "fetch",
        [shape(w.shape, w.dtype) for w in fetched],
        fetched,
        [pltpu.SemaphoreType.DMA((2 * FETCH_PIECES,))],
        [pl.BlockSpec(memory_space=pltpu.HBM)] * 2,
        100000,
    )
    *blocks, gathered = project(
        functools.partial(first_kernel, n_dt, n_kv, names),
        "first",
        (gate, up),
        (residual_input, *arrived, leading_norm_gain.reshape(1, width)),
    )
    parts = total_parts(down(hidden_rows(blocks, units), leading_down_weight, "first_down"))

    mixed = (query_projector, key_projector, forget_weight, value_projector, output_gate_weight)
    *blocks, after_first = project(
        functools.partial(project_kernel, 0.5, len(parts), len(mixed)),
        "attention_in",
        mixed,
        (gathered, *parts, attention_norm_gain.reshape(1, width)),
    )
    blocks = collect(blocks)
    heads = incoming_state.shape[1]
    keys, values = heads * KEY_CHANNELS, heads * VALUE_DIM
    upright = (padded(keys), padded(3 * height))
    head_rows, upright, value_rows = call(
        functools.partial(attention_kernel, features, n_kv),
        "attention",
        [shape((height, values), BF16), shape(upright, F32), shape((height, values), F32)],
        (*blocks, extra_log_decay, incoming_state, head_norm_gain.reshape(1, VALUE_DIM)),
        [pltpu.VMEM((height, values), F32), pltpu.VMEM(upright[::-1], F32)],
    )
    known = gather_rows(head_rows)
    outs = [shape(incoming_state.shape, F32), shape((8, LANES), F32)]
    new_state, finished = call(state_kernel, "state", outs, (upright, value_rows, incoming_state), work=100000)
    parts = total_parts(down(known, output_projector, "attention_out", finished))

    last = (trailing_gate_weight, trailing_up_weight)
    *blocks, second = project(
        functools.partial(project_kernel, 1.0, len(parts), len(last)),
        "last",
        last,
        (after_first, *parts, trailing_norm_gain.reshape(1, width)),
    )
    hidden = hidden_rows(blocks, units)
    parts = call(
        functools.partial(scatter_down_kernel, n_kv, names),
        "last_down",
        [shape((height, width), BF16)] * n_dt,
        (*hidden, trailing_down_weight),
        [pltpu.VMEM((rows, trailing_down_weight.shape[0]), BF16), pltpu.VMEM((rows, width), BF16)],
    )
    parts = [parts[0]] + swaps(parts[1:], dt, n_dt)
    result = call(
        functools.partial(result_kernel, n_dt, names), "result", shape((height, width), BF16), (second, *parts)
    )
    return (result, new_state)


def solution(mesh):
    n_dt = mesh.shape["dp"] * mesh.shape["tp"]
    n_kv = mesh.shape["kv"]
    assert n_dt == n_kv and n_kv & (n_kv - 1) == 0
    return jax.shard_map(
        functools.partial(per_device, n_dt, n_kv),
        mesh=mesh,
        in_specs=(
            P(("grp", "dp", "tp"), "kv"),
            P(("grp", "kv"), ("dp", "tp"), None, None),
            P(("grp", "kv"), ("dp", "tp")),
            P("kv"),
            P("kv", ("dp", "tp")),
            P("kv", ("dp", "tp")),
            P(("dp", "tp"), "kv"),
            P("kv"),
            P("kv", ("dp", "tp")),
            P("kv", ("dp", "tp")),
            P("kv", ("dp", "tp")),
            P("kv", ("dp", "tp")),
            P("kv", ("dp", "tp")),
            P(),
            P(("dp", "tp"), "kv"),
            P("kv"),
            P("kv", ("dp", "tp")),
            P("kv", ("dp", "tp")),
            P(("dp", "tp"), "kv"),
        ),
        out_specs=(P(("grp", "dp", "tp"), "kv"), P(("grp", "kv"), ("dp", "tp"), None, None)),
        check_vma=False,
    )
```

```python
import functools

import jax
import jax.numpy as jnp
from jax import lax
from jax.experimental import pallas as pl
from jax.experimental.pallas import tpu as pltpu
from jax.sharding import PartitionSpec as P

KEY_CHANNELS = 64
VALUE_DIM = 128
EPSILON = 1e-06
LANES = 128
F32 = jnp.float32
BF16 = jnp.bfloat16

VMEM = pl.BlockSpec(memory_space=pltpu.VMEM)


def padded(width):
    return -(-width // LANES) * LANES


def column_step(width):
    return 256 if width % 256 == 0 else width


def linear_index(axes):
    place = 0
    for axis in axes:
        place = place * lax.axis_size(axis) + lax.axis_index(axis)
    return place


def rows_at(block, height):
    return pl.ds(pl.multiple_of(block * height, height), height)


def swap(array, axes, size, offset):
    return lax.ppermute(array, axes, [(i, i ^ offset) for i in range(size)])


def swaps(arrays, axes, size):
    return [swap(array, axes, size, k + 1) for k, array in enumerate(arrays)]


def split_square_sum(total):
    high = total.astype(BF16).astype(F32)
    lane = lax.broadcasted_iota(jnp.int32, (total.shape[0], LANES), 1)
    return jnp.where(lane < LANES // 2, high, total - high)


def join_square_sum(block):
    return block[:, :1] + block[:, LANES // 2 : LANES // 2 + 1]


def fetch_kernel(n_weights, *refs):
    weights, outs, semaphores = refs[:n_weights], refs[n_weights : 2 * n_weights], refs[-1]
    copies = []
    for weight, out in zip(weights, outs):
        step = weight.shape[0] // FETCH_PIECES
        for piece in range(FETCH_PIECES):
            part = pl.ds(piece * step, step)
            copies.append(pltpu.make_async_copy(weight.at[part], out.at[part], semaphores.at[len(copies)]))
            copies[-1].start()
    for copy in copies:
        copy.wait()


def multiply_blocks(scaled, weight, columns, base, outs):
    height = outs[0].shape[0]
    first, width = columns
    step = column_step(width)
    for low in range(0, width, step):
        piece = weight[:, first + low : first + low + step]
        product = jnp.dot(scaled, piece, preferred_element_type=F32)
        for k, out in enumerate(outs):
            block = product[k * height : (k + 1) * height]
            out[:, base + low : base + low + step] = block.astype(out.dtype)


def put_squares(squares, low, outs):
    height = outs[0].shape[0]
    block = split_square_sum(squares)
    for k, out in enumerate(outs):
        out[:, low : low + LANES] = block[k * height : (k + 1) * height].astype(out.dtype)


def project_rows(scaled, weights, columns, outs):
    base = 0
    for weight in weights:
        span = columns or (0, weight.shape[1])
        multiply_blocks(scaled, weight, span, base, outs)
        base += padded(span[1])
    return base


def project_with_squares(widened, gain, weights, columns, outs):
    scaled = (widened * gain[...]).astype(BF16)
    base = project_rows(scaled, weights, columns, outs)
    put_squares(jnp.sum(widened * widened, axis=1, keepdims=True), base, outs)
    return scaled


def first_kernel(n_dt, n_kv, names, columns, *refs):
    own, others, refs = refs[0], refs[1:n_dt], refs[n_dt:]
    gain, weights, refs = refs[0], refs[1:3], refs[3:]
    outs, (gathered, scaled) = refs[:n_kv], refs[n_kv:]
    height = own.shape[0]
    place = linear_index(names[0]) ^ linear_index(names[1])
    for k, block in enumerate((own, *others)):
        gathered[rows_at(place ^ k, height), :] = block[...]
    scaled[...] = project_with_squares(gathered[...].astype(F32), gain, weights, columns, outs)


def last_kernel(n_parts, columns, *refs):
    residual, parts, refs = refs[0], refs[1 : 1 + n_parts], refs[1 + n_parts :]
    gain, weights, (*outs, stream, scaled) = refs[0], refs[1:3], refs[3:]
    stream[...] = add_parts(residual, parts, 1.0)
    scaled[...] = project_with_squares(stream[...].astype(F32), gain, weights, columns, outs)


def more_kernel(columns, scaled, gate, up, *outs):
    project_rows(scaled[...], (gate, up), columns, outs)


def add_parts(residual, parts, half):
    total = parts[0][...].astype(F32)
    for part in parts[1:]:
        total = total + part[...].astype(F32)
    return (residual[...].astype(F32) + half * total).astype(BF16)


def project_kernel(half, n_parts, n_weights, *refs):
    residual, parts, refs = refs[0], refs[1 : 1 + n_parts], refs[1 + n_parts :]
    gain, weights, refs = refs[0], refs[1 : 1 + n_weights], refs[1 + n_weights :]
    outs, stream = refs[:-1], refs[-1]
    stream[...] = add_parts(residual, parts, half)
    project_with_squares(stream[...].astype(F32), gain, weights, None, outs)


def sum_columns(parts, low, size):
    total = parts[0][:, low : low + size].astype(F32)
    for part in parts[1:]:
        total = total + part[:, low : low + size].astype(F32)
    return total


def hidden_kernel(features, n_kv, *refs):
    parts, out, scale = refs[:n_kv], refs[n_kv], refs[n_kv + 1]
    squares = join_square_sum(sum_columns(parts, 2 * padded(out.shape[1]), LANES))
    factor = lax.rsqrt(squares / features + EPSILON)
    scale[...] = jnp.broadcast_to(factor, scale.shape)
    activate(factor, parts, out)


def more_hidden_kernel(n_kv, *refs):
    activate(refs[n_kv][:, :1], refs[:n_kv], refs[n_kv + 1])


def activate(scale, parts, out):
    width = out.shape[1]
    gap = padded(width)
    step = column_step(width)
    for low in range(0, width, step):
        gate = jax.nn.silu(scale * sum_columns(parts, low, step))
        out[:, low : low + step] = (gate * (scale * sum_columns(parts, gap + low, step))).astype(BF16)


def stack_rows(blocks, rows):
    height = blocks[0].shape[0]
    for k, block in enumerate(blocks):
        rows[k * height : (k + 1) * height, :] = block[...]


def multiply_down(rows, weight, first_row, out, addend=None):
    step = column_step(weight.shape[1])
    for low in range(0, weight.shape[1], step):
        piece = weight[first_row : first_row + rows.shape[1], low : low + step]
        product = jnp.dot(rows[...], piece, preferred_element_type=F32)
        if addend is not None:
            product = product + addend[:, low : low + step]
        out[:, low : low + step] = product.astype(out.dtype)


def down_kernel(n_blocks, *refs):
    blocks, (weight, out, rows) = refs[:n_blocks], refs[n_blocks:]
    stack_rows(blocks, rows)
    multiply_down(rows, weight, 0, out)


def more_down_kernel(n_blocks, first_row, *refs):
    blocks, (weight, addend, out, rows) = refs[:n_blocks], refs[n_blocks:]
    stack_rows(blocks, rows)
    multiply_down(rows, weight, first_row, out, addend)


def scatter_down_kernel(n_blocks, first_row, names, *refs):
    blocks, (weight, addend), refs = refs[:n_blocks], refs[n_blocks : n_blocks + 2], refs[n_blocks + 2 :]
    outs, (rows, product) = refs[:-2], refs[-2:]
    stack_rows(blocks, rows)
    multiply_down(rows, weight, first_row, product, addend)
    height = blocks[0].shape[0]
    place = linear_index(names[0]) ^ linear_index(names[1])
    for k, out in enumerate(outs):
        out[...] = product[rows_at(place ^ k, height), :]


def attention_kernel(features, n_parts, *refs):
    parts, refs = refs[:n_parts], refs[n_parts:]
    extra_decay, state, norm_gain, head_rows, upright, value_rows, read, columns = refs
    rows, heads = state.shape[0], state.shape[1]
    keys, values = heads * KEY_CHANNELS, heads * VALUE_DIM
    gap, value_gap = padded(keys), padded(values)
    scale = lax.rsqrt(join_square_sum(sum_columns(parts, 3 * gap + 2 * value_gap, LANES)) / features + EPSILON)
    queries = scale * sum_columns(parts, 0, keys) * KEY_CHANNELS ** (-0.5)
    key_rows = scale * sum_columns(parts, gap, keys)
    forget = scale * sum_columns(parts, 2 * gap, keys)
    value_rows[...] = scale * sum_columns(parts, 3 * gap, values)
    log_sigmoid = jnp.minimum(forget, 0.0) - jnp.log1p(jnp.exp(-jnp.abs(forget)))
    decay = jnp.exp(log_sigmoid / 16.0 + extra_decay[...])
    columns[...] = jnp.zeros_like(columns)
    columns[0:rows, :keys] = decay
    columns[rows : 2 * rows, :keys] = key_rows
    columns[2 * rows : 3 * rows, :keys] = queries * decay
    upright[...] = columns[...].T
    matched = queries * key_rows
    for head in range(heads):
        channels = slice(head * KEY_CHANNELS, (head + 1) * KEY_CHANNELS)
        lanes = slice(head * VALUE_DIM, (head + 1) * VALUE_DIM)
        match = jnp.sum(matched[:, channels], axis=1, keepdims=True)
        for row in range(rows):
            taken = upright[channels, 2 * rows + row : 2 * rows + row + 1] * state[row, head]
            read[row : row + 1, lanes] = jnp.sum(taken, axis=0, keepdims=True)
        one = read[:, lanes] + match * value_rows[:, lanes]
        mean = jnp.mean(one * one, axis=-1, keepdims=True)
        normed = one * lax.rsqrt(mean + EPSILON) * norm_gain[...]
        low = 3 * gap + value_gap + head * VALUE_DIM
        gates = scale * sum_columns(parts, low, VALUE_DIM)
        head_rows[:, lanes] = (normed * jax.nn.silu(gates)).astype(BF16)


def state_kernel(upright, value_rows, state, new_state, finished):
    finished[...] = jnp.zeros_like(finished)
    rows, heads = state.shape[0], state.shape[1]
    for head in range(heads):
        channels = slice(head * KEY_CHANNELS, (head + 1) * KEY_CHANNELS)
        lanes = slice(head * VALUE_DIM, (head + 1) * VALUE_DIM)
        for row in range(rows):
            kept = upright[channels, row : row + 1] * state[row, head]
            added = upright[channels, rows + row : rows + row + 1] * value_rows[row : row + 1, lanes]
            new_state[row, head] = kept + added


def result_kernel(n_parts, names, *refs):
    stream, parts, out = refs[0], refs[1 : 1 + n_parts], refs[1 + n_parts]
    total = parts[0][...].astype(F32)
    for part in parts[1:]:
        total = total + part[...].astype(F32)
    place = linear_index(names[0]) ^ linear_index(names[1])
    own = stream[rows_at(place, out.shape[0]), :].astype(F32)
    out[...] = (own + 0.5 * total).astype(BF16)


MIB = 1 << 20
FETCH_PIECES = 4


def array_bytes(array):
    *lead, width = array.shape
    size = array.dtype.itemsize * padded(width)
    for extent in lead:
        size *= extent
    return size


def call(kernel, name, outs, inputs, scratch=(), in_specs=None, work=0, after=()):
    arrays = [*inputs, *jax.tree.leaves(outs)]

    def body(*refs):
        kernel(*refs[: len(inputs)], *refs[len(inputs) + len(after) :])

    return pl.pallas_call(
        body,
        out_shape=outs,
        in_specs=(in_specs or [VMEM] * len(inputs)) + [pl.BlockSpec(memory_space=pl.ANY)] * len(after),
        out_specs=jax.tree.map(lambda _: VMEM, outs),
        scratch_shapes=list(scratch),
        compiler_params=pltpu.CompilerParams(vmem_limit_bytes=sum(map(array_bytes, arrays)) + 8 * MIB),
        cost_estimate=pl.CostEstimate(flops=work, bytes_accessed=0, transcendentals=0),
        name=name,
    )(*inputs, *after)


def per_device(
    n_dt,
    n_kv,
    residual_input,
    incoming_state,
    extra_log_decay,
    leading_norm_gain,
    leading_gate_weight,
    leading_up_weight,
    leading_down_weight,
    attention_norm_gain,
    query_projector,
    key_projector,
    value_projector,
    output_gate_weight,
    forget_weight,
    head_norm_gain,
    output_projector,
    trailing_norm_gain,
    trailing_gate_weight,
    trailing_up_weight,
    trailing_down_weight,
):
    dt, kv = ("dp", "tp"), ("kv",)
    names = (dt, kv)
    height, width = residual_input.shape
    features = width * n_kv
    rows = height * n_dt
    shape = jax.ShapeDtypeStruct

    def collect(blocks):
        return [blocks[0]] + swaps(blocks[1:], kv, n_kv)

    def gather_rows(block):
        return [block] + [swap(block, kv, n_kv, k) for k in range(1, n_kv)]

    def total_parts(part):
        offset = n_dt // 2
        while offset > 1:
            part = (part.astype(F32) + swap(part, dt, n_dt, offset).astype(F32)).astype(BF16)
            offset //= 2
        return [part, swap(part, dt, n_dt, offset)]

    def row_blocks(span):
        return [shape((height, span), F32)] + [shape((height, span), BF16)] * (n_kv - 1)

    def stack(unit):
        return [pltpu.VMEM((rows, unit), BF16)]

    def mixer(kernel, name, inputs, weights, down_weight, finish, finish_outs, finish_scratch):
        units = weights[0].shape[1]
        near = min(-(-units // 2 // 256) * 256, units)
        rest = units - near
        *blocks, stream, scaled = call(
            functools.partial(kernel, (0, near)),
            name,
            row_blocks(2 * padded(near) + LANES) + [shape((rows, width), BF16)] * 2,
            (*inputs, *weights),
        )
        more = call(
            functools.partial(more_kernel, (near, rest)), name + "_more", row_blocks(2 * padded(rest)), (scaled, *weights)
        )
        outs = [shape((height, near), BF16), shape((height, LANES), F32)]
        parts = collect(blocks)
        more_parts = collect(more)
        hidden, scale = call(functools.partial(hidden_kernel, features, n_kv), "hidden", outs, parts)
        hidden = gather_rows(hidden)
        more_hidden = call(
            functools.partial(more_hidden_kernel, n_kv), "hidden_more", shape((height, rest), BF16), (*more_parts, scale)
        )
        more_hidden = gather_rows(more_hidden)
        product = call(
            functools.partial(down_kernel, n_kv), name + "_down", shape((rows, width), F32), (*hidden, down_weight), stack(near)
        )
        return stream, call(
            functools.partial(finish, n_kv, near),
            name + "_down_more",
            finish_outs,
            (*more_hidden, down_weight, product),
            stack(rest) + finish_scratch,
        )

    def down(blocks, weight, name, *after):
        kernel = functools.partial(down_kernel, n_kv)
        inputs = (*blocks, weight)
        return call(kernel, name, shape((rows, weight.shape[1]), BF16), inputs, stack(weight.shape[0]), after=after)

    arrived = [swap(residual_input, dt, n_dt, k) for k in range(1, n_dt)]
    fetched = [
        pltpu.with_memory_space_constraint(w, pltpu.HBM) for w in (leading_gate_weight, leading_up_weight)
    ]
    gate, up = call(
        functools.partial(fetch_kernel, 2),
        "fetch",
        [shape(w.shape, w.dtype) for w in fetched],
        fetched,
        [pltpu.SemaphoreType.DMA((2 * FETCH_PIECES,))],
        [pl.BlockSpec(memory_space=pltpu.HBM)] * 2,
        100000,
    )
    whole_rows = shape((rows, width), BF16)
    gathered, part = mixer(
        functools.partial(first_kernel, n_dt, n_kv, names),
        "first",
        (residual_input, *arrived, leading_norm_gain.reshape(1, width)),
        (gate, up),
        leading_down_weight,
        more_down_kernel,
        whole_rows,
        [],
    )
    parts = total_parts(part)

    mixed = (query_projector, key_projector, forget_weight, value_projector, output_gate_weight)
    span = sum(padded(w.shape[1]) for w in mixed) + LANES
    *blocks, after_first = call(
        functools.partial(project_kernel, 0.5, len(parts), len(mixed)),
        "attention_in",
        row_blocks(span) + [whole_rows],
        (gathered, *parts, attention_norm_gain.reshape(1, width), *mixed),
    )
    blocks = collect(blocks)
    heads = incoming_state.shape[1]
    keys, values = heads * KEY_CHANNELS, heads * VALUE_DIM
    upright = (padded(keys), padded(3 * height))
    head_rows, upright, value_rows = call(
        functools.partial(attention_kernel, features, n_kv),
        "attention",
        [shape((height, values), BF16), shape(upright, F32), shape((height, values), F32)],
        (*blocks, extra_log_decay, incoming_state, head_norm_gain.reshape(1, VALUE_DIM)),
        [pltpu.VMEM((height, values), F32), pltpu.VMEM(upright[::-1], F32)],
    )
    known = gather_rows(head_rows)
    outs = [shape(incoming_state.shape, F32), shape((8, LANES), F32)]
    new_state, finished = call(state_kernel, "state", outs, (upright, value_rows, incoming_state), work=100000)
    parts = total_parts(down(known, output_projector, "attention_out", finished))

    second, parts = mixer(
        functools.partial(last_kernel, len(parts)),
        "last",
        (after_first, *parts, trailing_norm_gain.reshape(1, width)),
        (trailing_gate_weight, trailing_up_weight),
        trailing_down_weight,
        lambda n_blocks, first_row, *refs: scatter_down_kernel(n_blocks, first_row, names, *refs),
        [shape((height, width), BF16)] * n_dt,
        [pltpu.VMEM((rows, width), BF16)],
    )
    parts = [parts[0]] + swaps(parts[1:], dt, n_dt)
    result = call(
        functools.partial(result_kernel, n_dt, names), "result", shape((height, width), BF16), (second, *parts)
    )
    return (result, new_state)


def solution(mesh):
    n_dt = mesh.shape["dp"] * mesh.shape["tp"]
    n_kv = mesh.shape["kv"]
    assert n_dt == n_kv and n_kv & (n_kv - 1) == 0
    return jax.shard_map(
        functools.partial(per_device, n_dt, n_kv),
        mesh=mesh,
        in_specs=(
            P(("grp", "dp", "tp"), "kv"),
            P(("grp", "kv"), ("dp", "tp"), None, None),
            P(("grp", "kv"), ("dp", "tp")),
            P("kv"),
            P("kv", ("dp", "tp")),
            P("kv", ("dp", "tp")),
            P(("dp", "tp"), "kv"),
            P("kv"),
            P("kv", ("dp", "tp")),
            P("kv", ("dp", "tp")),
            P("kv", ("dp", "tp")),
            P("kv", ("dp", "tp")),
            P("kv", ("dp", "tp")),
            P(),
            P(("dp", "tp"), "kv"),
            P("kv"),
            P("kv", ("dp", "tp")),
            P("kv", ("dp", "tp")),
            P(("dp", "tp"), "kv"),
        ),
        out_specs=(P(("grp", "dp", "tp"), "kv"), P(("grp", "kv"), ("dp", "tp"), None, None)),
        check_vma=False,
    )
```

```python
import functools

import jax
import jax.numpy as jnp
from jax import lax
from jax.experimental import pallas as pl
from jax.experimental.pallas import tpu as pltpu
from jax.sharding import PartitionSpec as P

KEY_CHANNELS = 64
VALUE_DIM = 128
EPSILON = 1e-06
LANES = 128
F32 = jnp.float32
BF16 = jnp.bfloat16

VMEM = pl.BlockSpec(memory_space=pltpu.VMEM)


def padded(width):
    return -(-width // LANES) * LANES


def column_step(width):
    return 256 if width % 256 == 0 else width


def linear_index(axes):
    place = 0
    for axis in axes:
        place = place * lax.axis_size(axis) + lax.axis_index(axis)
    return place


def rows_at(block, height):
    return pl.ds(pl.multiple_of(block * height, height), height)


def swap(array, axes, size, offset):
    return lax.ppermute(array, axes, [(i, i ^ offset) for i in range(size)])


def swaps(arrays, axes, size):
    return [swap(array, axes, size, k + 1) for k, array in enumerate(arrays)]


def split_square_sum(total):
    high = total.astype(BF16).astype(F32)
    lane = lax.broadcasted_iota(jnp.int32, (total.shape[0], LANES), 1)
    return jnp.where(lane < LANES // 2, high, total - high)


def join_square_sum(block):
    return block[:, :1] + block[:, LANES // 2 : LANES // 2 + 1]


def fetch_kernel(n_weights, first, *refs):
    weights, outs, semaphores = refs[:n_weights], refs[n_weights : 2 * n_weights], refs[-1]
    copies = []
    for weight, out in zip(weights, outs):
        step = weight.shape[0] // FETCH_PIECES
        for piece in range(FETCH_PIECES):
            part = pl.ds(piece * step, step)
            source = weight.at[part, pl.ds(first, out.shape[1])]
            copies.append(pltpu.make_async_copy(source, out.at[part], semaphores.at[len(copies)]))
            copies[-1].start()
    for copy in copies:
        copy.wait()


def multiply_blocks(scaled, weight, columns, base, outs):
    height = outs[0].shape[0]
    first, width = columns
    step = column_step(width)
    for low in range(0, width, step):
        piece = weight[:, first + low : first + low + step]
        product = jnp.dot(scaled, piece, preferred_element_type=F32)
        for k, out in enumerate(outs):
            block = product[k * height : (k + 1) * height]
            out[:, base + low : base + low + step] = block.astype(out.dtype)


def put_squares(squares, low, outs):
    height = outs[0].shape[0]
    block = split_square_sum(squares)
    for k, out in enumerate(outs):
        out[:, low : low + LANES] = block[k * height : (k + 1) * height].astype(out.dtype)


def project_rows(scaled, weights, columns, outs):
    base = 0
    for weight in weights:
        span = columns or (0, weight.shape[1])
        multiply_blocks(scaled, weight, span, base, outs)
        base += padded(span[1])
    return base


def project_with_squares(widened, gain, weights, columns, outs):
    scaled = (widened * gain[...]).astype(BF16)
    base = project_rows(scaled, weights, columns, outs)
    put_squares(jnp.sum(widened * widened, axis=1, keepdims=True), base, outs)
    return scaled


def first_kernel(n_dt, n_kv, names, columns, *refs):
    own, others, refs = refs[0], refs[1:n_dt], refs[n_dt:]
    gain, weights, refs = refs[0], refs[1:3], refs[3:]
    outs, (gathered, scaled) = refs[:n_kv], refs[n_kv:]
    height = own.shape[0]
    place = linear_index(names[0]) ^ linear_index(names[1])
    for k, block in enumerate((own, *others)):
        gathered[rows_at(place ^ k, height), :] = block[...]
    scaled[...] = project_with_squares(gathered[...].astype(F32), gain, weights, columns, outs)


def last_kernel(n_parts, columns, *refs):
    residual, parts, refs = refs[0], refs[1 : 1 + n_parts], refs[1 + n_parts :]
    gain, weights, (*outs, stream, scaled) = refs[0], refs[1:3], refs[3:]
    stream[...] = add_parts(residual, parts, 1.0)
    scaled[...] = project_with_squares(stream[...].astype(F32), gain, weights, columns, outs)


def more_kernel(columns, scaled, gate, up, *outs):
    project_rows(scaled[...], (gate, up), columns, outs)


def add_parts(residual, parts, half):
    total = parts[0][...].astype(F32)
    for part in parts[1:]:
        total = total + part[...].astype(F32)
    return (residual[...].astype(F32) + half * total).astype(BF16)


def project_kernel(half, n_parts, n_weights, *refs):
    residual, parts, refs = refs[0], refs[1 : 1 + n_parts], refs[1 + n_parts :]
    gain, weights, refs = refs[0], refs[1 : 1 + n_weights], refs[1 + n_weights :]
    outs, stream = refs[:-1], refs[-1]
    stream[...] = add_parts(residual, parts, half)
    project_with_squares(stream[...].astype(F32), gain, weights, None, outs)


def sum_columns(parts, low, size):
    total = parts[0][:, low : low + size].astype(F32)
    for part in parts[1:]:
        total = total + part[:, low : low + size].astype(F32)
    return total


def hidden_kernel(features, n_kv, *refs):
    parts, out, scale = refs[:n_kv], refs[n_kv], refs[n_kv + 1]
    squares = join_square_sum(sum_columns(parts, 2 * padded(out.shape[1]), LANES))
    factor = lax.rsqrt(squares / features + EPSILON)
    scale[...] = jnp.broadcast_to(factor, scale.shape)
    activate(factor, parts, out)


def more_hidden_kernel(n_kv, *refs):
    activate(refs[n_kv][:, :1], refs[:n_kv], refs[n_kv + 1])


def activate(scale, parts, out):
    width = out.shape[1]
    gap = padded(width)
    step = column_step(width)
    for low in range(0, width, step):
        gate = jax.nn.silu(scale * sum_columns(parts, low, step))
        out[:, low : low + step] = (gate * (scale * sum_columns(parts, gap + low, step))).astype(BF16)


def stack_rows(blocks, rows):
    height = blocks[0].shape[0]
    for k, block in enumerate(blocks):
        rows[k * height : (k + 1) * height, :] = block[...]


def multiply_down(rows, weight, first_row, out, addend=None):
    step = column_step(weight.shape[1])
    for low in range(0, weight.shape[1], step):
        piece = weight[first_row : first_row + rows.shape[1], low : low + step]
        product = jnp.dot(rows[...], piece, preferred_element_type=F32)
        if addend is not None:
            product = product + addend[:, low : low + step]
        out[:, low : low + step] = product.astype(out.dtype)


def down_kernel(n_blocks, *refs):
    blocks, (weight, out, rows) = refs[:n_blocks], refs[n_blocks:]
    stack_rows(blocks, rows)
    multiply_down(rows, weight, 0, out)


def more_down_kernel(n_blocks, first_row, *refs):
    blocks, (weight, addend, out, rows) = refs[:n_blocks], refs[n_blocks:]
    stack_rows(blocks, rows)
    multiply_down(rows, weight, first_row, out, addend)


def scatter_down_kernel(n_blocks, first_row, names, *refs):
    blocks, (weight, addend), refs = refs[:n_blocks], refs[n_blocks : n_blocks + 2], refs[n_blocks + 2 :]
    outs, (rows, product) = refs[:-2], refs[-2:]
    stack_rows(blocks, rows)
    multiply_down(rows, weight, first_row, product, addend)
    height = blocks[0].shape[0]
    place = linear_index(names[0]) ^ linear_index(names[1])
    for k, out in enumerate(outs):
        out[...] = product[rows_at(place ^ k, height), :]


def attention_kernel(features, n_parts, *refs):
    parts, refs = refs[:n_parts], refs[n_parts:]
    extra_decay, state, norm_gain, head_rows, upright, value_rows, read, columns = refs
    rows, heads = state.shape[0], state.shape[1]
    keys, values = heads * KEY_CHANNELS, heads * VALUE_DIM
    gap, value_gap = padded(keys), padded(values)
    scale = lax.rsqrt(join_square_sum(sum_columns(parts, 3 * gap + 2 * value_gap, LANES)) / features + EPSILON)
    queries = scale * sum_columns(parts, 0, keys) * KEY_CHANNELS ** (-0.5)
    key_rows = scale * sum_columns(parts, gap, keys)
    forget = scale * sum_columns(parts, 2 * gap, keys)
    value_rows[...] = scale * sum_columns(parts, 3 * gap, values)
    log_sigmoid = jnp.minimum(forget, 0.0) - jnp.log1p(jnp.exp(-jnp.abs(forget)))
    decay = jnp.exp(log_sigmoid / 16.0 + extra_decay[...])
    columns[...] = jnp.zeros_like(columns)
    columns[0:rows, :keys] = decay
    columns[rows : 2 * rows, :keys] = key_rows
    columns[2 * rows : 3 * rows, :keys] = queries * decay
    upright[...] = columns[...].T
    matched = queries * key_rows
    for head in range(heads):
        channels = slice(head * KEY_CHANNELS, (head + 1) * KEY_CHANNELS)
        lanes = slice(head * VALUE_DIM, (head + 1) * VALUE_DIM)
        match = jnp.sum(matched[:, channels], axis=1, keepdims=True)
        for row in range(rows):
            taken = upright[channels, 2 * rows + row : 2 * rows + row + 1] * state[row, head]
            read[row : row + 1, lanes] = jnp.sum(taken, axis=0, keepdims=True)
        one = read[:, lanes] + match * value_rows[:, lanes]
        mean = jnp.mean(one * one, axis=-1, keepdims=True)
        normed = one * lax.rsqrt(mean + EPSILON) * norm_gain[...]
        low = 3 * gap + value_gap + head * VALUE_DIM
        gates = scale * sum_columns(parts, low, VALUE_DIM)
        head_rows[:, lanes] = (normed * jax.nn.silu(gates)).astype(BF16)


def state_kernel(upright, value_rows, state, new_state, finished):
    finished[...] = jnp.zeros_like(finished)
    rows, heads = state.shape[0], state.shape[1]
    for head in range(heads):
        channels = slice(head * KEY_CHANNELS, (head + 1) * KEY_CHANNELS)
        lanes = slice(head * VALUE_DIM, (head + 1) * VALUE_DIM)
        for row in range(rows):
            kept = upright[channels, row : row + 1] * state[row, head]
            added = upright[channels, rows + row : rows + row + 1] * value_rows[row : row + 1, lanes]
            new_state[row, head] = kept + added


def result_kernel(n_parts, names, *refs):
    stream, parts, out = refs[0], refs[1 : 1 + n_parts], refs[1 + n_parts]
    total = parts[0][...].astype(F32)
    for part in parts[1:]:
        total = total + part[...].astype(F32)
    place = linear_index(names[0]) ^ linear_index(names[1])
    own = stream[rows_at(place, out.shape[0]), :].astype(F32)
    out[...] = (own + 0.5 * total).astype(BF16)


MIB = 1 << 20
FETCH_PIECES = 4
NEAR_SHARE = 2


def first_chunk(units):
    return min(-(-units * NEAR_SHARE // 1024) * 256, units)


def array_bytes(array):
    *lead, width = array.shape
    size = array.dtype.itemsize * padded(width)
    for extent in lead:
        size *= extent
    return size


def call(kernel, name, outs, inputs, scratch=(), in_specs=None, work=0, after=()):
    arrays = [*inputs, *jax.tree.leaves(outs)]

    def body(*refs):
        kernel(*refs[: len(inputs)], *refs[len(inputs) + len(after) :])

    return pl.pallas_call(
        body,
        out_shape=outs,
        in_specs=(in_specs or [VMEM] * len(inputs)) + [pl.BlockSpec(memory_space=pl.ANY)] * len(after),
        out_specs=jax.tree.map(lambda _: VMEM, outs),
        scratch_shapes=list(scratch),
        compiler_params=pltpu.CompilerParams(vmem_limit_bytes=sum(map(array_bytes, arrays)) + 8 * MIB),
        cost_estimate=pl.CostEstimate(flops=work, bytes_accessed=0, transcendentals=0),
        name=name,
    )(*inputs, *after)


def per_device(
    n_dt,
    n_kv,
    residual_input,
    incoming_state,
    extra_log_decay,
    leading_norm_gain,
    leading_gate_weight,
    leading_up_weight,
    leading_down_weight,
    attention_norm_gain,
    query_projector,
    key_projector,
    value_projector,
    output_gate_weight,
    forget_weight,
    head_norm_gain,
    output_projector,
    trailing_norm_gain,
    trailing_gate_weight,
    trailing_up_weight,
    trailing_down_weight,
):
    dt, kv = ("dp", "tp"), ("kv",)
    names = (dt, kv)
    height, width = residual_input.shape
    features = width * n_kv
    rows = height * n_dt
    shape = jax.ShapeDtypeStruct

    def collect(blocks):
        return [blocks[0]] + swaps(blocks[1:], kv, n_kv)

    def gather_rows(block):
        return [block] + [swap(block, kv, n_kv, k) for k in range(1, n_kv)]

    def total_parts(part):
        offset = n_dt // 2
        while offset > 1:
            part = (part.astype(F32) + swap(part, dt, n_dt, offset).astype(F32)).astype(BF16)
            offset //= 2
        return [part, swap(part, dt, n_dt, offset)]

    def row_blocks(span):
        return [shape((height, span), F32)] + [shape((height, span), BF16)] * (n_kv - 1)

    def stack(unit):
        return [pltpu.VMEM((rows, unit), BF16)]

    def mixer(kernel, name, inputs, weights, more_weights, down_weight, finish, finish_outs, finish_scratch):
        units = down_weight.shape[0]
        near = first_chunk(units)
        rest = units - near
        *blocks, stream, scaled = call(
            kernel,
            name,
            row_blocks(2 * padded(near) + LANES) + [shape((rows, width), BF16)] * 2,
            (*inputs, *weights),
        )
        if callable(more_weights):
            more_weights, columns = more_weights(scaled), None
        else:
            columns = (near, rest)
        more = call(
            functools.partial(more_kernel, columns),
            name + "_more",
            row_blocks(2 * padded(rest)),
            (scaled, *more_weights),
        )
        outs = [shape((height, near), BF16), shape((height, LANES), F32)]
        parts = collect(blocks)
        more_parts = collect(more)
        hidden, scale = call(functools.partial(hidden_kernel, features, n_kv), "hidden", outs, parts)
        hidden = gather_rows(hidden)
        more_hidden = call(
            functools.partial(more_hidden_kernel, n_kv), "hidden_more", shape((height, rest), BF16), (*more_parts, scale)
        )
        more_hidden = gather_rows(more_hidden)
        product = call(
            functools.partial(down_kernel, n_kv), name + "_down", shape((rows, width), F32), (*hidden, down_weight), stack(near)
        )
        return stream, call(
            functools.partial(finish, n_kv, near),
            name + "_down_more",
            finish_outs,
            (*more_hidden, down_weight, product),
            stack(rest) + finish_scratch,
        )

    def down(blocks, weight, name, *after):
        kernel = functools.partial(down_kernel, n_kv)
        inputs = (*blocks, weight)
        return call(kernel, name, shape((rows, weight.shape[1]), BF16), inputs, stack(weight.shape[0]), after=after)

    arrived = [swap(residual_input, dt, n_dt, k) for k in range(1, n_dt)]
    def fetch(weights, first, size, after):
        return call(
            functools.partial(fetch_kernel, len(weights), first),
            "fetch",
            [shape((w.shape[0], size), w.dtype) for w in weights],
            [pltpu.with_memory_space_constraint(w, pltpu.HBM) for w in weights],
            [pltpu.SemaphoreType.DMA((len(weights) * FETCH_PIECES,))],
            [pl.BlockSpec(memory_space=pltpu.HBM)] * len(weights),
            100000,
            after,
        )

    units = leading_gate_weight.shape[1]
    near = first_chunk(units)
    first = (leading_gate_weight, leading_up_weight)
    whole_rows = shape((rows, width), BF16)
    gathered, part = mixer(
        functools.partial(first_kernel, n_dt, n_kv, names, None),
        "first",
        (residual_input, *arrived, leading_norm_gain.reshape(1, width)),
        fetch(first, 0, near, ()),
        lambda scaled: fetch(first, near, units - near, (scaled,)),
        leading_down_weight,
        more_down_kernel,
        whole_rows,
        [],
    )
    parts = total_parts(part)

    mixed = (query_projector, key_projector, forget_weight, value_projector, output_gate_weight)
    span = sum(padded(w.shape[1]) for w in mixed) + LANES
    *blocks, after_first = call(
        functools.partial(project_kernel, 0.5, len(parts), len(mixed)),
        "attention_in",
        row_blocks(span) + [whole_rows],
        (gathered, *parts, attention_norm_gain.reshape(1, width), *mixed),
    )
    blocks = collect(blocks)
    heads = incoming_state.shape[1]
    keys, values = heads * KEY_CHANNELS, heads * VALUE_DIM
    upright = (padded(keys), padded(3 * height))
    head_rows, upright, value_rows = call(
        functools.partial(attention_kernel, features, n_kv),
        "attention",
        [shape((height, values), BF16), shape(upright, F32), shape((height, values), F32)],
        (*blocks, extra_log_decay, incoming_state, head_norm_gain.reshape(1, VALUE_DIM)),
        [pltpu.VMEM((height, values), F32), pltpu.VMEM(upright[::-1], F32)],
    )
    known = gather_rows(head_rows)
    outs = [shape(incoming_state.shape, F32), shape((8, LANES), F32)]
    new_state, finished = call(state_kernel, "state", outs, (upright, value_rows, incoming_state), work=100000)
    parts = total_parts(down(known, output_projector, "attention_out", finished))

    last = (trailing_gate_weight, trailing_up_weight)
    second, parts = mixer(
        functools.partial(last_kernel, len(parts), (0, near)),
        "last",
        (after_first, *parts, trailing_norm_gain.reshape(1, width)),
        last,
        last,
        trailing_down_weight,
        lambda n_blocks, first_row, *refs: scatter_down_kernel(n_blocks, first_row, names, *refs),
        [shape((height, width), BF16)] * n_dt,
        [pltpu.VMEM((rows, width), BF16)],
    )
    parts = [parts[0]] + swaps(parts[1:], dt, n_dt)
    result = call(
        functools.partial(result_kernel, n_dt, names), "result", shape((height, width), BF16), (second, *parts)
    )
    return (result, new_state)


def solution(mesh):
    n_dt = mesh.shape["dp"] * mesh.shape["tp"]
    n_kv = mesh.shape["kv"]
    assert n_dt == n_kv and n_kv & (n_kv - 1) == 0
    return jax.shard_map(
        functools.partial(per_device, n_dt, n_kv),
        mesh=mesh,
        in_specs=(
            P(("grp", "dp", "tp"), "kv"),
            P(("grp", "kv"), ("dp", "tp"), None, None),
            P(("grp", "kv"), ("dp", "tp")),
            P("kv"),
            P("kv", ("dp", "tp")),
            P("kv", ("dp", "tp")),
            P(("dp", "tp"), "kv"),
            P("kv"),
            P("kv", ("dp", "tp")),
            P("kv", ("dp", "tp")),
            P("kv", ("dp", "tp")),
            P("kv", ("dp", "tp")),
            P("kv", ("dp", "tp")),
            P(),
            P(("dp", "tp"), "kv"),
            P("kv"),
            P("kv", ("dp", "tp")),
            P("kv", ("dp", "tp")),
            P(("dp", "tp"), "kv"),
        ),
        out_specs=(P(("grp", "dp", "tp"), "kv"), P(("grp", "kv"), ("dp", "tp"), None, None)),
        check_vma=False,
    )
```
